32 devices in a mesh: grp: 2 (over y), sp: 4 (over z), tp: 4 (over x, core).
Axes of the slice: x: 2, y: 2, z: 4, core: 2. Of those that a mesh axis runs over, the one named last changes fastest.
Arguments:
- tokens: bfloat16 [2048, 8, 2048], P('sp', 'grp'), parts along dimension 1, may hold values from -48 to 48
- query_weight: bfloat16 [2048, 1024], P(None, 'tp'), may hold values from -2 to 2
- key_weight: bfloat16 [2048, 1024], P(None, 'tp'), may hold values from -2 to 2
- value_weight: bfloat16 [2048, 1024], P(None, 'tp'), may hold values from -3 to 3
- mix_gain: float32 [1024], P('tp'), may hold values from 0.1 to 1.9
- out_weight: bfloat16 [1024, 2048], P('tp'), may hold values from -0.1875 to 0.1875
Outputs:
- mixed: bfloat16 [2048, 8, 2048], P(('sp', 'tp'), 'grp'), parts along dimension 1
The draws below stay inside these ranges and needn't reach their ends.
There are 2 independent parts, one for each index of `grp`. The reference program is written for one: setup_inputs(seed, part) draws one part's arguments, and reference() takes and returns one part's arrays. A program takes and returns all parts, laid end to end along the dimension named above; an argument that names none is the same for every part. Nothing has to cross between parts.
All inputs are finite; a program needn't handle non-finite values.
Results may differ from the reference program's by a relative error of at most 0.02.
Values may be sent and summed in bfloat16 or wider, within the bound.
A program may use at most 128 MiB of HBM per device.

```python
import jax
import jax.numpy as jnp
from jax import lax

D = 2048
HEADS = 16
HEAD_DIM = 64
A_W = 1024
BATCH = 4
SEQ = 2048
N_TP = 4


def draw_tokens(key, part):
    normal_part = jax.random.normal(jax.random.fold_in(key, 1), (SEQ, BATCH, D), jnp.float32)
    result = jnp.clip(normal_part, -6.0, 6.0)
    return result.astype(jnp.bfloat16)


def projection_pair(key):
    leading = jnp.clip(jax.random.normal(jax.random.fold_in(key, 11), (D, A_W), jnp.float32), -6.0, 6.0)
    partner = jnp.clip(jax.random.normal(jax.random.fold_in(key, 12), (D, A_W), jnp.float32), -6.0, 6.0)
    return (leading * D ** (-0.5), partner * D ** (-0.5))


def draw_query_weight(key, part):
    leading, partner = projection_pair(key)
    return leading.astype(jnp.bfloat16)


def draw_key_weight(key, part):
    leading, partner = projection_pair(key)
    blended = partner
    return blended.astype(jnp.bfloat16)


def draw_value_weight(key, part):
    normal_part = jnp.clip(jax.random.normal(jax.random.fold_in(key, 21), (D, A_W), jnp.float32), -6.0, 6.0)
    factors = jnp.exp(jax.random.uniform(jax.random.fold_in(key, 22), (HEADS,), jnp.float32, -1.1, 1.1))
    scaled = normal_part * D ** (-0.5) * jnp.repeat(factors, HEAD_DIM)[None, :]
    return scaled.astype(jnp.bfloat16)


def levels(rng, shape, split, smallest, high):
    loudness, own = 1.0, jax.random.fold_in(rng, 6)
    for dim, shards_of in split:
        draws = jnp.exp(jax.random.uniform(jax.random.fold_in(own, dim), (shards_of,), jnp.float32, smallest / len(split), high / len(split)))
        loudness = loudness * jnp.repeat(draws, shape[dim] // shards_of).reshape([-1 if axis == dim else 1 for axis in range(len(shape))])
    return loudness


def bell_draw(rng, extent, spread, most, shards=(), held_as=jnp.bfloat16):
    loudness = levels(rng, extent, shards, -0.22, 0.18) if shards else 1.0
    entries = jax.random.normal(rng, extent, jnp.float32) * spread * loudness
    return jnp.minimum(jnp.maximum(entries, -most), most).astype(held_as)


def setup_inputs(seed: int = 0, part: int = 0) -> dict:
    streams_of = jax.random.split(jax.random.key(seed), 7)
    part_keys = jax.random.split(jax.random.fold_in(streams_of[6], part), 7)
    return {
        "tokens": draw_tokens(jax.random.fold_in(jax.random.fold_in(streams_of[6], part), 71), part),
        "query_weight": draw_query_weight(jax.random.fold_in(streams_of[6], 71), part),
        "key_weight": draw_key_weight(jax.random.fold_in(streams_of[6], 71), part),
        "value_weight": draw_value_weight(jax.random.fold_in(streams_of[6], 71), part),
        "mix_gain": jnp.clip(1.0 + 0.18 * jax.random.normal(streams_of[4], (A_W,), jnp.float32), 0.1, 1.9),
        "out_weight": bell_draw(streams_of[5], (A_W, D), A_W ** -0.5, 0.1875, ((0, 4),)),
    }


PATTERNS = ((128, 1), (512, 4), (2048, 16))
REACH = 128
EPSILON = 1e-06
NEGATIVE = -1e+30

def band_attend(queries, key_rows, value_rows, live_mask):
    lead_shape = queries.shape[:3]
    query_len = queries.shape[3]
    head_size = queries.shape[4]
    block_len = min(REACH, query_len)
    block_count = query_len // block_len
    query_blocks = queries.reshape(lead_shape + (block_count, block_len, head_size))
    if block_count == 1:
        key_ctx = key_rows.reshape(lead_shape + (1, query_len + REACH, head_size))
        value_ctx = value_rows.reshape(lead_shape + (1, query_len + REACH, head_size))
        live_ctx = live_mask.reshape((live_mask.shape[0], 1, query_len + REACH))
    else:
        key_blocks = key_rows.reshape(lead_shape + (block_count + 1, REACH, head_size))
        value_blocks = value_rows.reshape(lead_shape + (block_count + 1, REACH, head_size))
        key_ctx = jnp.concatenate([key_blocks[:, :, :, :-1], key_blocks[:, :, :, 1:]], axis=4)
        value_ctx = jnp.concatenate([value_blocks[:, :, :, :-1], value_blocks[:, :, :, 1:]], axis=4)
        live_blocks = live_mask.reshape((live_mask.shape[0], block_count + 1, REACH))
        live_ctx = jnp.concatenate([live_blocks[:, :-1], live_blocks[:, 1:]], axis=2)
    ctx_width = block_len + REACH
    offset = jnp.arange(ctx_width)[None, :] - jnp.arange(block_len)[:, None]
    in_band = (offset >= 0) & (offset <= REACH)
    valid = in_band[None, None] & live_ctx[:, :, None, :]
    scores = jnp.einsum('gbhnqe,gbhnke->gbhnqk', query_blocks.astype(jnp.float32), key_ctx.astype(jnp.float32)) * head_size ** (-0.5)
    scores = jnp.where(valid[:, None, None], scores, NEGATIVE)
    highest = lax.optimization_barrier(jnp.max(scores, axis=-1, keepdims=True))
    raised = jnp.exp(scores - highest)
    totals = lax.optimization_barrier(jnp.sum(raised, axis=-1, keepdims=True))
    probs = (raised / totals).astype(jnp.bfloat16)
    result = jnp.einsum('gbhnqk,gbhnke->gbhnqe', probs.astype(jnp.float32), value_ctx.astype(jnp.float32)).astype(jnp.bfloat16)
    log_norm = (highest + jnp.log(totals))[..., 0]
    return (result.reshape(lead_shape + (query_len, head_size)), log_norm.reshape(lead_shape + (query_len,)))

def dilated_pattern(queries, context, base, window, stride):
    seq_rows, batch_size, channels = queries.shape
    heads_dev = channels // HEAD_DIM
    query_len = seq_rows // stride
    key_len = query_len + REACH
    query_class = queries.reshape(query_len, stride, batch_size, heads_dev, HEAD_DIM).transpose(1, 2, 3, 0, 4)
    keyval_class = context.reshape(key_len, stride, batch_size, 2 * heads_dev, HEAD_DIM).transpose(1, 2, 3, 0, 4)
    position = jnp.arange(key_len)[None, :] * stride + jnp.arange(stride)[:, None] + base
    result, log_norm = band_attend(query_class, keyval_class[:, :, :heads_dev], keyval_class[:, :, heads_dev:], position >= 0)
    result = result.transpose(3, 0, 1, 2, 4).reshape(seq_rows, batch_size, channels)
    log_norm = log_norm.transpose(3, 0, 1, 2).reshape(seq_rows, batch_size, heads_dev)
    return (result, log_norm)

def reference(tokens, query_weight, key_weight, value_weight, mix_gain, out_weight):
    seq_len, batch_size, width = tokens.shape
    flat = tokens.reshape(seq_len * batch_size, width)

    def project(weight):
        product = jnp.dot(flat, weight, preferred_element_type=jnp.float32).astype(jnp.bfloat16)
        return product.reshape(seq_len, batch_size, weight.shape[1])
    queries = project(query_weight)
    key_values = jnp.concatenate([project(key_weight), project(value_weight)], axis=-1)
    channels = queries.shape[2]
    heads_all = channels // HEAD_DIM

    def one_sequence(pair):
        query_seq, keyval_seq = pair
        query_seq = query_seq[:, None]
        keyval_seq = keyval_seq[:, None]
        results = []
        norms = []
        for window, stride in PATTERNS:
            context = jnp.pad(keyval_seq, ((window, 0), (0, 0), (0, 0)))
            result, log_norm = dilated_pattern(query_seq, context, -window, window, stride)
            results.append(result)
            norms.append(log_norm)
        weights = jax.nn.softmax(jnp.stack(norms, axis=0), axis=0)
        combined = jnp.zeros((seq_len, 1, heads_all, HEAD_DIM), jnp.float32)
        for index in range(len(PATTERNS)):
            combined = combined + weights[index][..., None] * results[index].astype(jnp.float32).reshape(seq_len, 1, heads_all, HEAD_DIM)
        return combined.reshape(seq_len, channels)
    combined = lax.map(one_sequence, (queries.transpose(1, 0, 2), key_values.transpose(1, 0, 2)))
    combined = combined.transpose(1, 0, 2)
    mean_square = lax.optimization_barrier(jnp.sum(combined * combined, axis=-1, keepdims=True)) / channels
    normed = (combined * lax.rsqrt(mean_square + EPSILON) * mix_gain.astype(jnp.float32)).astype(jnp.bfloat16)
    group = channels // N_TP
    total = jnp.zeros((seq_len * batch_size, out_weight.shape[1]), jnp.float32)
    for member in range(N_TP):
        block = normed[..., member * group:(member + 1) * group].reshape(seq_len * batch_size, group)
        partial_out = jnp.dot(block, out_weight[member * group:(member + 1) * group], preferred_element_type=jnp.float32).astype(jnp.bfloat16)
        total = total + partial_out.astype(jnp.float32)
    return total.reshape(seq_len, batch_size, out_weight.shape[1]).astype(jnp.bfloat16)
```

```python
import functools

import jax
import jax.numpy as jnp
from jax import lax
from jax.experimental import pallas as pl
from jax.experimental.pallas import tpu as pltpu
from jax.sharding import PartitionSpec as P

HEAD_DIM = 64
PATTERNS = ((128, 1), (512, 4), (2048, 16))
REACH = 128
CLASSES = 16
LANES = 128
EPSILON = 1e-06
NEGATIVE = -1e30
GROUPS = 2


def attend_kernel(q_ref, k_ref, v_ref, o_ref, out_sc, top_sc, sum_sc, near_bias, mid_bias, far_bias):
    chunks, _, per_class, width = q_ref.shape
    heads = width // HEAD_DIM
    tile = 16
    near_rows = CLASSES * tile
    mid_rows = 4 * per_class
    span = REACH // per_class
    far_tiles = chunks // span

    def bias_of(diff, window, live):
        return jnp.where((diff >= 0) & (diff <= window) & live, 0.0, NEGATIVE).astype(jnp.float32)

    row = lax.broadcasted_iota(jnp.int32, near_bias.shape[1:], 0)
    col = lax.broadcasted_iota(jnp.int32, near_bias.shape[1:], 1)
    diff = (row % tile - col % tile) * 16 + row // tile - (col % near_rows) // tile
    diff = diff + jnp.where(col < near_rows, near_rows, 0)
    near_bias[0] = bias_of(diff, PATTERNS[0][0], col >= near_rows)
    near_bias[1] = bias_of(diff, PATTERNS[0][0], col >= 0)
    row = lax.broadcasted_iota(jnp.int32, mid_bias.shape[1:], 0)
    col = lax.broadcasted_iota(jnp.int32, mid_bias.shape[1:], 1)
    diff = (row % per_class - col % per_class) * 16
    diff = diff + 4 * (row // per_class - (col % mid_rows) // per_class)
    diff = diff + jnp.where(col < mid_rows, CLASSES * per_class, 0)
    mid_bias[0] = bias_of(diff, PATTERNS[1][0], col >= mid_rows)
    mid_bias[1] = bias_of(diff, PATTERNS[1][0], col >= 0)
    row = lax.broadcasted_iota(jnp.int32, far_bias.shape, 0)
    col = lax.broadcasted_iota(jnp.int32, far_bias.shape, 1)
    far_bias[...] = bias_of(row + REACH - col, REACH, col >= 0)

    lane = lax.broadcasted_iota(jnp.int32, (1, width), 1) // HEAD_DIM
    picks = [jnp.where(lane == h, HEAD_DIM ** -0.5, 0.0).astype(jnp.bfloat16) for h in range(heads)]

    def attend(queries, keys, values, bias):
        outs, tops, sums = [], [], []
        for h in range(heads):
            scores = lax.dot_general(
                queries * picks[h], keys, (((1,), (1,)), ((), ())), preferred_element_type=jnp.float32
            ) + bias
            top = jnp.max(scores, axis=1, keepdims=True)
            raised = jnp.exp(scores - top)
            total = jnp.sum(raised, axis=1, keepdims=True)
            outs.append(jnp.dot(raised.astype(jnp.bfloat16), values, preferred_element_type=jnp.float32))
            tops.append(jnp.broadcast_to(top, outs[-1].shape))
            sums.append(jnp.broadcast_to(total, outs[-1].shape))

        def join(parts):
            whole = parts[0]
            for h in range(1, heads):
                whole = jnp.where(lane == h, parts[h], whole)
            return whole

        return join(outs), join(tops), join(sums)

    def merge_rows(ref, *index):
        block = ref[index]
        return block.reshape(-1, width)

    @pl.loop(0, chunks)
    def near_and_mid(z):
        before = jnp.maximum(z - 1, 0)
        first = jnp.minimum(z, 1)
        for u in range(per_class // tile):
            rows = slice(u * tile, (u + 1) * tile)
            back, back_rows, kind = (before, slice(per_class - tile, per_class), first)
            if u > 0:
                back, back_rows, kind = (z, slice((u - 1) * tile, u * tile), 1)
            queries = q_ref[z, :, rows, :].reshape(near_rows, width)
            keys, values = (
                jnp.concatenate(
                    [
                        ref[back, :, back_rows, :].reshape(near_rows, width),
                        ref[z, :, rows, :].reshape(near_rows, width),
                    ],
                    axis=0,
                )
                for ref in (k_ref, v_ref)
            )
            for ref, part in zip((out_sc, top_sc, sum_sc), attend(queries, keys, values, near_bias[kind])):
                ref[0, z, :, rows, :] = part.reshape(CLASSES, tile, width)
        for r in range(4):
            classes = range(r, CLASSES, 4)
            queries = jnp.concatenate([q_ref[z, c] for c in classes], axis=0)
            keys, values = (
                jnp.concatenate([ref[y, c] for y in (before, z) for c in classes], axis=0)
                for ref in (k_ref, v_ref)
            )
            for ref, part in zip((out_sc, top_sc, sum_sc), attend(queries, keys, values, mid_bias[first])):
                for m, c in enumerate(classes):
                    ref[1, z, c] = part[m * per_class : (m + 1) * per_class]

    @pl.loop(0, CLASSES // 4)
    def far(quad):
        for inner in range(4):
            c = quad * 4 + inner
            for n in range(far_tiles):
                here = slice(n * span, (n + 1) * span)
                reach = slice(max(n - 1, 0) * span, (n + 1) * span)
                queries = q_ref[here, c].reshape(REACH, width)
                keys, values = (ref[reach, c].reshape(-1, width) for ref in (k_ref, v_ref))
                bias = far_bias[...] if n > 0 else far_bias[:, REACH:]
                for ref, part in zip((out_sc, top_sc, sum_sc), attend(queries, keys, values, bias)):
                    ref[2, here, c] = part.reshape(span, per_class, width)

    @pl.loop(0, chunks)
    def mix(z):
        tops = [top_sc[p, z] for p in range(3)]
        highest = jnp.maximum(jnp.maximum(tops[0], tops[1]), tops[2])
        lifts = [jnp.exp(top - highest) for top in tops]
        total = sum(lift * sum_sc[p, z] for p, lift in enumerate(lifts))
        result = sum(lift * out_sc[p, z] for p, lift in enumerate(lifts))
        o_ref[z] = (result / total).astype(o_ref.dtype)


def attend_all(moved, width):
    chunks, batches, _, per_class, triple = moved.shape
    channels = triple // 3
    pairs = channels // width
    if width % 128 == 0:
        operands = (moved, moved, moved)
        starts = (0, pairs, 2 * pairs)
    else:
        operands = tuple(moved[..., i * channels : (i + 1) * channels] for i in range(3))
        starts = (0, 0, 0)
    block = (chunks, None, CLASSES, per_class, width)
    tokens = chunks * CLASSES * per_class
    return pl.pallas_call(
        attend_kernel,
        grid=(batches, pairs),
        in_specs=[
            pl.BlockSpec(block, functools.partial(lambda s, b, i: (0, b, 0, 0, s + i), start)) for start in starts
        ],
        out_specs=pl.BlockSpec(block, lambda b, i: (0, b, 0, 0, i)),
        out_shape=jax.ShapeDtypeStruct((chunks, batches, CLASSES, per_class, channels), jnp.bfloat16),
        scratch_shapes=[pltpu.VMEM((3, chunks, CLASSES, per_class, width), jnp.float32) for _ in range(3)]
        + [
            pltpu.VMEM((2, 256, 512), jnp.float32),
            pltpu.VMEM((2, 4 * per_class, 8 * per_class), jnp.float32),
            pltpu.VMEM((REACH, 2 * REACH), jnp.float32),
        ],
        cost_estimate=pl.CostEstimate(
            flops=tokens * batches * channels * 4 * 900,
            bytes_accessed=tokens * batches * channels * 8,
            transcendentals=tokens * batches * channels // HEAD_DIM * 900,
        ),
    )(*operands)


def project_kernel(weight_count, places, tokens_ref, *refs):
    weight_refs, out_ref, product = refs[:weight_count], refs[weight_count], refs[-1]
    step = pl.program_id(0)
    positions, batch_size, features = tokens_ref.shape
    rows = positions * batch_size
    flat = tokens_ref[...].reshape(rows, features)
    at = pl.ds(pl.multiple_of(step * rows, rows), rows)
    for weight_ref, parts in zip(weight_refs, places):
        total = jnp.dot(flat, weight_ref[...], preferred_element_type=jnp.float32)
        for i, part in enumerate(parts):
            product[part, at, :] = total[:, i * LANES : (i + 1) * LANES]

    @pl.when(step == pl.num_programs(0) - 1)
    def leave():
        per_class = out_ref.shape[2]

        @pl.loop(0, CLASSES)
        def of_class(c):
            for part in range(product.shape[0]):
                for b in range(batch_size):
                    picked = pl.ds(c * batch_size + b, per_class, stride=CLASSES * batch_size)
                    out_ref[b, c, :, part * LANES : (part + 1) * LANES] = product[part, picked, :].astype(out_ref.dtype)


def project(tokens, weights, group, cut):
    seq_rows, batch_size, features = tokens.shape
    columns = cut * len(weights)
    per_class = seq_rows // CLASSES
    block = min(64, seq_rows)
    shape = (batch_size, CLASSES, per_class, columns)
    each = cut // LANES
    places = [range(w * each, (w + 1) * each) for w in range(len(weights))]
    return pl.pallas_call(
        functools.partial(project_kernel, len(weights), places),
        grid=(seq_rows // block,),
        in_specs=[pl.BlockSpec((block, batch_size, features), lambda i: (i, 0, 0))]
        + [pl.BlockSpec((features, cut), lambda i: (0, group))] * len(weights),
        out_specs=pl.BlockSpec(shape, lambda i: (0, 0, 0, 0)),
        out_shape=jax.ShapeDtypeStruct(shape, jnp.bfloat16),
        scratch_shapes=[pltpu.VMEM((columns // LANES, seq_rows * batch_size, LANES), jnp.float32)],
        compiler_params=pltpu.CompilerParams(dimension_semantics=("arbitrary",)),
        cost_estimate=pl.CostEstimate(
            flops=2 * seq_rows * batch_size * features * columns,
            bytes_accessed=2 * (tokens.size + features * columns + seq_rows * batch_size * columns),
            transcendentals=0,
        ),
    )(tokens, *weights)


STRIDE = PATTERNS[1][1]
MESH = pl.DeviceIdType.MESH


def split_kernel(pairs, tokens_ref, *refs):
    weight_refs, out_ref, product = refs[:3], refs[3], refs[4]
    step = pl.program_id(0)
    positions, batch_size, features = tokens_ref.shape
    rows = positions * batch_size
    flat = tokens_ref[...].reshape(rows, features)
    at = pl.ds(pl.multiple_of(step * rows, rows), rows)
    for which, weight_ref in enumerate(weight_refs):
        total = jnp.dot(flat, weight_ref[...], preferred_element_type=jnp.float32)
        for pair in range(pairs):
            product[which * pairs + pair, at, :] = total[:, pair * LANES : (pair + 1) * LANES]

    @pl.when(step == pl.num_programs(0) - 1)
    def leave():
        per = out_ref.shape[2] // STRIDE

        @pl.loop(0, STRIDE)
        def of_class(r):
            here = pl.ds(pl.multiple_of(r * per, per), per)
            for b in range(batch_size):
                picked = pl.ds(r * batch_size + b, per, stride=STRIDE * batch_size)
                for which in range(3):
                    for pair in range(pairs):
                        out_ref[pair * batch_size + b, which, here, :] = product[
                            which * pairs + pair, picked, :
                        ].astype(out_ref.dtype)


def split_project(tokens, weights):
    seq_rows, batch_size, features = tokens.shape
    channels = weights[0].shape[1]
    pairs = channels // LANES
    block = min(64, seq_rows)
    shape = (pairs * batch_size, 3, seq_rows, LANES)
    return pl.pallas_call(
        functools.partial(split_kernel, pairs),
        grid=(seq_rows // block,),
        in_specs=[pl.BlockSpec((block, batch_size, features), lambda i: (i, 0, 0))]
        + [pl.BlockSpec((features, channels), lambda i: (0, 0))] * 3,
        out_specs=pl.BlockSpec(shape, lambda i: (0, 0, 0, 0)),
        out_shape=jax.ShapeDtypeStruct(shape, jnp.bfloat16),
        scratch_shapes=[pltpu.VMEM((3 * pairs, seq_rows * batch_size, LANES), jnp.float32)],
        compiler_params=pltpu.CompilerParams(dimension_semantics=("arbitrary",)),
        cost_estimate=pl.CostEstimate(
            flops=6 * seq_rows * batch_size * features * channels,
            bytes_accessed=2 * (tokens.size + 3 * features * channels + 3 * seq_rows * batch_size * channels),
            transcendentals=0,
        ),
    )(tokens, *weights)


def layer_kernel(pairs, batch_size, qkv_ref, own_ref, out_ref, *scratch):
    (late_q, last_q, first_kv, back, back_norm, sent, sent_norm, held, held_norm, done, gathered, weights, normed,
     diag_bias, class_bias, corner_bias, send_sem, recv_sem, part_send, part_recv, w_send, w_recv) = scratch
    place = lax.axis_index("sp")
    member = lax.axis_index("tp")
    pieces = qkv_ref.shape[0]
    chunk = qkv_ref.shape[2]
    per = chunk // STRIDE
    tail = REACH // STRIDE
    members = gathered.shape[0]
    share = per // members
    half = LANES // 2

    barrier = pltpu.get_barrier_semaphore()
    for other in range(1, 4):
        pl.semaphore_signal(barrier, inc=1, device_id={"sp": lax.rem(place + other, 4)}, device_id_type=MESH)
        pl.semaphore_signal(barrier, inc=1, device_id={"tp": member ^ other}, device_id_type=MESH)
    pl.semaphore_wait(barrier, 6)

    def to_place(kind, i, src, dst, target, axis="sp"):
        return pltpu.make_async_remote_copy(
            src_ref=src, dst_ref=dst, send_sem=send_sem.at[kind, i], recv_sem=recv_sem.at[kind, i],
            device_id={axis: target}, device_id_type=MESH,
        )

    def copy_kv(i):
        return to_place(0, i, qkv_ref.at[i, pl.ds(1, 2)], first_kv.at[i], 1)

    def copy_q2(i):
        return to_place(1, i, qkv_ref.at[i, 0], late_q.at[i], 1)

    def copy_q3(i, target):
        return to_place(1 + target, i, qkv_ref.at[i, 0], last_q.at[i], target)

    def copy_back(i, slot, source_slot, target):
        kind = 4 + target - 2 + 2 * slot
        return (
            to_place(kind, i, sent.at[source_slot, i], back.at[slot, i], target),
            to_place(kind + 4, i, sent_norm.at[source_slot, i], back_norm.at[slot, i], target),
        )

    def copy_part(i, x):
        rows = pl.ds(pl.multiple_of((member ^ x) * share, share), share)
        return pltpu.make_async_remote_copy(
            src_ref=done.at[i, :, rows], dst_ref=gathered.at[member, i],
            send_sem=part_send.at[x - 1, i], recv_sem=part_recv.at[x - 1, i],
            device_id={"tp": member ^ x}, device_id_type=MESH,
        )

    def copy_weight(x, kind):
        src = own_ref if kind < 2 else weights.at[member ^ 2]
        dst = weights.at[member ^ 2 if kind == 2 else member]
        return pltpu.make_async_remote_copy(
            src_ref=src, dst_ref=dst, send_sem=w_send.at[kind], recv_sem=w_recv.at[kind],
            device_id={"tp": member ^ x}, device_id_type=MESH,
        )

    @pl.when(place == 0)
    def send_first():
        @pl.loop(0, pieces)
        def one(i):
            copy_kv(i).start()

    @pl.when(place == 2)
    def send_late():
        @pl.loop(0, pieces)
        def one(i):
            copy_q2(i).start()

    @pl.when(place == 3)
    def send_last():
        @pl.loop(0, pieces)
        def one(i):
            copy_q3(i, 1).start()
            copy_q3(i, 2).start()

    copy_weight(2, 0).start()
    copy_weight(1, 1).start()

    def bias_of(diff, patterns):
        count = jnp.zeros(diff.shape, jnp.int32)
        for window, dilation in patterns:
            count += jnp.where((diff >= 0) & (diff <= window) & (diff % dilation == 0), 1, 0)
        logs = jnp.where(count == 2, 0.6931471805599453, jnp.where(count == 3, 1.0986122886681098, 0.0))
        return jnp.where(count == 0, NEGATIVE, logs).astype(jnp.float32)

    row = lax.broadcasted_iota(jnp.int32, (chunk, LANES), 0)
    col = lax.broadcasted_iota(jnp.int32, (chunk, LANES), 1)
    for r in range(STRIDE):
        diag_bias[r] = bias_of(STRIDE * (col - row % per) + r - row // per, PATTERNS)
        key = row[:REACH]
        back_by = STRIDE * (per - tail + key % tail) + key // tail
        corner_bias[r] = bias_of(chunk + STRIDE * col[:REACH] + r - back_by, PATTERNS[:1])
    for gap in range(2):
        class_bias[gap] = bias_of((gap + 1) * chunk + STRIDE * (col[:per] - row[:per]), PATTERNS[1:])

    lane = lax.broadcasted_iota(jnp.int32, (1, LANES), 1) // HEAD_DIM
    picks = [jnp.where(lane == h, HEAD_DIM ** -0.5, 0.0).astype(jnp.bfloat16) for h in range(2)]
    eye = jnp.where(
        lax.broadcasted_iota(jnp.int32, (LANES, LANES), 0) == lax.broadcasted_iota(jnp.int32, (LANES, LANES), 1), 1.0, 0.0
    ).astype(jnp.bfloat16)

    def contract_last(a, b):
        return lax.dot_general(a, b, (((1,), (1,)), ((), ())), preferred_element_type=jnp.float32)

    def turn(a):
        return contract_last(eye, a).astype(jnp.bfloat16)

    def spread(two):
        return jnp.concatenate([jnp.broadcast_to(two[h : h + 1], (half, LANES)) for h in range(2)], axis=0)

    def attend(queries, parts):
        both = jnp.concatenate([queries * picks[0], queries * picks[1]], axis=0)
        scores = []
        for keys, _, bias in parts:
            scores.append(contract_last(keys, both) + jnp.concatenate([bias, bias], axis=1))
        top = functools.reduce(jnp.maximum, [jnp.max(s, axis=0, keepdims=True) for s in scores])
        total, result = 0.0, 0.0
        for s, (_, turned, _) in zip(scores, parts):
            raised = jnp.exp(s - top)
            total += jnp.sum(raised, axis=0, keepdims=True)
            result += jnp.dot(turned, raised.astype(jnp.bfloat16), preferred_element_type=jnp.float32)
        picked = jnp.concatenate([result[:half, :LANES], result[half:, LANES:]], axis=0)
        norm = top + jnp.log(total)
        inverse = 1.0 / total
        two = jnp.concatenate([inverse[:, :LANES], inverse[:, LANES:]], axis=0)
        return picked * spread(two), jnp.concatenate([norm[:, :LANES], norm[:, LANES:]], axis=0)

    def cls(r):
        return slice(r * per, (r + 1) * per)

    def corner_of(rows):
        return jnp.concatenate([rows[r * per + per - tail : (r + 1) * per] for r in range(STRIDE)], axis=0)

    def finish(i, r, result):
        done[i, r] = turn(result.astype(jnp.bfloat16)[...].reshape(LANES, LANES)).astype(jnp.bfloat16)

    def send_parts(i):
        mine = pl.ds(pl.multiple_of(member * share, share), share)
        gathered[member, i] = done[i, :, mine]
        for x in range(1, members):
            copy_part(i, x).start()

    def own_parts(i):
        return qkv_ref[i, 1], turn(qkv_ref[i, 2])

    def far_parts(keys, turned, r, gap):
        return keys[cls(r)], turned[:, cls(r)], class_bias[gap]

    def give_back(i, source_slot, slot, target, r, answer):
        sent[source_slot, i, :, cls(r)] = answer[0].astype(jnp.bfloat16)
        sent_norm[source_slot, i, :, cls(r)] = answer[1]

    def merge(i, sources):
        for r in range(STRIDE):
            norms = [held_norm[i, :, cls(r)]] + [back_norm[s, i, :, cls(r)] for s in sources]
            results = [held[i, :, cls(r)]] + [back[s, i, :, cls(r)].astype(jnp.float32) for s in sources]
            top = functools.reduce(jnp.maximum, norms)
            raised = [jnp.exp(n - top) for n in norms]
            inverse = 1.0 / sum(raised)
            finish(i, r, sum(spread(e * inverse) * o for e, o in zip(raised, results)))

    @pl.when(place == 0)
    def first():
        @pl.loop(0, pieces)
        def one(i):
            keys, turned = own_parts(i)
            for r in range(STRIDE):
                finish(i, r, attend(qkv_ref[i, 0, cls(r)], [(keys, turned, diag_bias[r])])[0])
            send_parts(i)

        @pl.loop(0, pieces)
        def sent_all(i):
            copy_kv(i).wait_send()

    @pl.when(place == 1)
    def second():
        @pl.loop(0, pieces)
        def one(i):
            keys, turned = own_parts(i)
            near_keys = corner_of(keys)
            near_turned = turn(corner_of(qkv_ref[i, 2]))
            copy_kv(i).wait_recv()
            old_keys, old_turned = first_kv[i, 0], turn(first_kv[i, 1])
            copy_q2(i).wait_recv()
            for r in range(STRIDE):
                parts = [
                    far_parts(keys, turned, r, 0),
                    (near_keys, near_turned, corner_bias[r]),
                    far_parts(old_keys, old_turned, r, 1),
                ]
                give_back(i, 0, 0, 2, r, attend(late_q[i, cls(r)], parts))
            for c in copy_back(i, 0, 0, 2):
                c.start()
            copy_q3(i, 1).wait_recv()
            for r in range(STRIDE):
                parts = [far_parts(keys, turned, r, 1), far_parts(old_keys, old_turned, r, 1)]
                give_back(i, 1, 0, 3, r, attend(last_q[i, cls(r)], parts))
            for c in copy_back(i, 0, 1, 3):
                c.start()
            old_near_keys = corner_of(old_keys)
            old_near_turned = turn(corner_of(first_kv[i, 1]))
            for r in range(STRIDE):
                parts = [
                    (keys, turned, diag_bias[r]),
                    far_parts(old_keys, old_turned, r, 0),
                    (old_near_keys, old_near_turned, corner_bias[r]),
                ]
                finish(i, r, attend(qkv_ref[i, 0, cls(r)], parts)[0])
            send_parts(i)

        @pl.loop(0, pieces)
        def sent_all(i):
            for c in copy_back(i, 0, 0, 2) + copy_back(i, 0, 1, 3):
                c.wait_send()

    @pl.when(place >= 2)
    def later():
        @pl.loop(0, pieces)
        def one(i):
            keys, turned = own_parts(i)
            for r in range(STRIDE):
                held[i, :, cls(r)], held_norm[i, :, cls(r)] = attend(
                    qkv_ref[i, 0, cls(r)], [(keys, turned, diag_bias[r])]
                )

            @pl.when(place == 2)
            def help_last():
                near_keys = corner_of(qkv_ref[i, 1])
                near_turned = turn(corner_of(qkv_ref[i, 2]))
                copy_q3(i, 2).wait_recv()
                for r in range(STRIDE):
                    parts = [far_parts(keys, turned, r, 0), (near_keys, near_turned, corner_bias[r])]
                    give_back(i, 0, 1, 3, r, attend(last_q[i, cls(r)], parts))
                for c in copy_back(i, 1, 0, 3):
                    c.start()

    copy_weight(2, 0).wait_recv()
    copy_weight(1, 2).start()

    @pl.when(place == 2)
    def third():
        @pl.loop(0, pieces)
        def one(i):
            for c in copy_back(i, 0, 0, 2):
                c.wait_recv()
            merge(i, (0,))
            send_parts(i)

        @pl.loop(0, pieces)
        def sent_all(i):
            copy_q2(i).wait_send()
            for c in copy_back(i, 1, 0, 3):
                c.wait_send()

    @pl.when(place == 3)
    def fourth():
        @pl.loop(0, pieces)
        def one(i):
            for c in copy_back(i, 0, 1, 3) + copy_back(i, 1, 0, 3):
                c.wait_recv()
            merge(i, (0, 1))
            send_parts(i)

        @pl.loop(0, pieces)
        def sent_all(i):
            copy_q3(i, 1).wait_send()
            copy_q3(i, 2).wait_send()

    @pl.loop(0, pieces)
    def parts_all(i):
        for x in range(1, members):
            copy_part(i, x).wait_send()
            copy_part(i, x).wait_recv()

    copy_weight(1, 1).wait_recv()
    copy_weight(1, 2).wait_recv()
    for x, kind in ((2, 0), (1, 1), (1, 2)):
        copy_weight(x, kind).wait_send()
    weights[member] = own_ref[...]

    rows = batch_size * STRIDE * share
    width = pairs * LANES
    blocks = [gathered[t, p * batch_size : (p + 1) * batch_size].reshape(rows, LANES)
              for t in range(members) for p in range(pairs)]
    target = lax.broadcasted_iota(jnp.int32, (rows, rows), 0)
    source = lax.broadcasted_iota(jnp.int32, (rows, rows), 1)
    moved_to = (source % share) * (STRIDE * batch_size) + (source // share % STRIDE) * batch_size
    moved_to = moved_to + source // (share * STRIDE)
    order = jnp.where(target == moved_to, 1.0, 0.0).astype(jnp.bfloat16)
    square = 0.0
    turned = []
    for block in blocks:
        turned.append(jnp.dot(order, block, preferred_element_type=jnp.float32))
        square += turned[-1] * turned[-1]
    square = jnp.sum(square, axis=1, keepdims=True)
    scale = lax.rsqrt(square * (1.0 / (LANES * len(blocks))) + EPSILON)
    for at, block in enumerate(turned):
        normed[:, at * LANES : (at + 1) * LANES] = (block * scale).astype(jnp.bfloat16)

    @pl.loop(0, out_ref.shape[1] // (2 * LANES))
    def project_out(n):
        columns = pl.ds(pl.multiple_of(n * 2 * LANES, 2 * LANES), 2 * LANES)
        total = 0.0
        for t in range(members):
            total += jnp.dot(
                normed[:, t * width : (t + 1) * width], weights[t, :, columns], preferred_element_type=jnp.float32
            )
        out_ref[:, columns] = total.astype(out_ref.dtype)


def layer(qkv, own, batch_size, members):
    pieces, _, chunk, _ = qkv.shape
    depth, columns = own.shape
    pairs = pieces // batch_size
    per = chunk // STRIDE
    rows = batch_size * chunk // members
    bf16, f32 = jnp.bfloat16, jnp.float32
    sems = pltpu.SemaphoreType.DMA
    return pl.pallas_call(
        functools.partial(layer_kernel, pairs, batch_size),
        in_specs=[pl.BlockSpec(memory_space=pltpu.VMEM)] * 2,
        out_specs=pl.BlockSpec(memory_space=pltpu.VMEM),
        out_shape=jax.ShapeDtypeStruct((rows, columns), bf16),
        scratch_shapes=[
            pltpu.VMEM((pieces, chunk, LANES), bf16),
            pltpu.VMEM((pieces, chunk, LANES), bf16),
            pltpu.VMEM((pieces, 2, chunk, LANES), bf16),
            pltpu.VMEM((2, pieces, LANES, chunk), bf16),
            pltpu.VMEM((2, pieces, 2, chunk), f32),
            pltpu.VMEM((2, pieces, LANES, chunk), bf16),
            pltpu.VMEM((2, pieces, 2, chunk), f32),
            pltpu.VMEM((pieces, LANES, chunk), f32),
            pltpu.VMEM((pieces, 2, chunk), f32),
            pltpu.VMEM((pieces, STRIDE, per, LANES), bf16),
            pltpu.VMEM((members, pieces, STRIDE, per // members, LANES), bf16),
            pltpu.VMEM((members, depth, columns), bf16),
            pltpu.VMEM((rows, depth * members), bf16),
            pltpu.VMEM((STRIDE, chunk, LANES), f32),
            pltpu.VMEM((2, per, LANES), f32),
            pltpu.VMEM((STRIDE, REACH, LANES), f32),
            sems((12, pieces)),
            sems((12, pieces)),
            sems((members - 1, pieces)),
            sems((members - 1, pieces)),
            sems((3,)),
            sems((3,)),
        ],
        compiler_params=pltpu.CompilerParams(collective_id=0, has_side_effects=True),
        cost_estimate=pl.CostEstimate(
            flops=2 * rows * columns * depth * members, bytes_accessed=2 * qkv.size, transcendentals=qkv.size * 100
        ),
    )(qkv, own)


def four_chunks(tokens, query_weight, key_weight, value_weight, mix_gain, out_weight):
    batch_size = tokens.shape[1]
    own = (out_weight.astype(jnp.float32) * mix_gain[:, None]).astype(jnp.bfloat16)
    qkv = split_project(tokens, (query_weight, key_weight, value_weight))
    mixed = layer(qkv, own, batch_size, lax.axis_size("tp"))
    return mixed.reshape(-1, batch_size, out_weight.shape[1])


def fits_four_chunks(tokens, query_weight):
    return (
        lax.axis_size("sp") == 4
        and lax.axis_size("tp") == 4
        and tokens.shape[0] == STRIDE * LANES
        and tokens.shape[0] == PATTERNS[1][0]
        and 4 * tokens.shape[0] <= PATTERNS[2][0]
        and query_weight.shape[1] % LANES == 0
    )


def body(tokens, query_weight, key_weight, value_weight, mix_gain, out_weight):
    if fits_four_chunks(tokens, query_weight):
        return four_chunks(tokens, query_weight, key_weight, value_weight, mix_gain, out_weight)
    seq_rows, batch_size, features = tokens.shape
    channels = query_weight.shape[1]
    sp_count = lax.axis_size("sp")
    tp_count = lax.axis_size("tp")
    tp_place = lax.axis_index("tp")
    per_class = seq_rows // CLASSES
    head_split = min(max(1, sp_count // batch_size), channels // HEAD_DIM)
    copies = max(1, sp_count // (batch_size * head_split))
    batches = max(1, batch_size // sp_count)
    groups = GROUPS if head_split == 1 else 1

    own = (out_weight.astype(jnp.float32) * mix_gain[:, None]).astype(jnp.bfloat16)
    gathered, sources, step = own, [0], tp_count // 2
    while step:
        route = [(i, i ^ step) for i in range(tp_count)]
        gathered = jnp.concatenate([gathered, lax.ppermute(gathered, "tp", route)], axis=0)
        sources += [s ^ step for s in sources]
        step //= 2

    cut = channels // groups // head_split
    width = min(cut, 2 * HEAD_DIM)
    weights = (query_weight, key_weight, value_weight)
    results = []
    for g in range(groups):
        if cut % LANES == 0 and head_split == 1:
            product = project(tokens, weights, g, cut)
        else:
            spans = [slice(i * cut, (i + 1) * cut) for i in range(g * head_split, (g + 1) * head_split)]
            whole = jnp.concatenate([w[:, span] for span in spans for w in weights], axis=1)
            product = project(tokens, (whole,), 0, whole.shape[1])
        if head_split > 1:
            product = product.reshape(batch_size, seq_rows, head_split, 3 * cut).transpose(0, 2, 1, 3)
        product = product.reshape(sp_count // copies, batches * seq_rows, 3 * cut)
        if copies > 1:
            product = jnp.repeat(product, copies, axis=0)
        moved = lax.all_to_all(product, "sp", split_axis=0, concat_axis=0, tiled=True)
        if g == 0:
            moved, gathered = lax.optimization_barrier((moved, gathered))
        moved = moved.reshape(sp_count, batches, CLASSES, per_class, 3 * cut)
        results.append(attend_all(moved, width))

    part = per_class // tp_count
    backs = []
    for result in results:
        back = result.reshape(sp_count, batches, CLASSES, tp_count, part, cut).transpose(0, 3, 1, 2, 4, 5)
        back = back.reshape(sp_count * tp_count, batches * CLASSES * part, cut)
        back = lax.all_to_all(back, ("sp", "tp"), split_axis=0, concat_axis=0, tiled=True)
        back = back.reshape(batch_size // batches, head_split, copies, tp_count, batches, CLASSES, part, cut)[:, :, 0]
        backs.append(back)
    combined = jnp.stack(backs, axis=0).transpose(3, 6, 5, 1, 4, 0, 2, 7)
    rows = part * CLASSES * batch_size
    combined = combined.reshape(tp_count, rows, channels)
    turned = jnp.concatenate(
        [lax.dynamic_index_in_dim(combined, tp_place ^ s, axis=0, keepdims=False) for s in sources], axis=1
    )
    wide = turned.astype(jnp.float32)
    row_scale = lax.rsqrt(jnp.mean(wide * wide, axis=-1, keepdims=True) + EPSILON)
    mixed = jnp.dot(turned, gathered, preferred_element_type=jnp.float32) * row_scale
    return mixed.astype(jnp.bfloat16).reshape(part * CLASSES, batch_size, out_weight.shape[1])


def solution(mesh):
    in_specs = (
        P("sp", "grp", None),
        P(None, "tp"),
        P(None, "tp"),
        P(None, "tp"),
        P("tp"),
        P("tp", None),
    )
    out_specs = P(("sp", "tp"), "grp", None)
    return jax.shard_map(body, mesh=mesh, in_specs=in_specs, out_specs=out_specs, check_vma=False)
```

```python
import functools

import jax
import jax.numpy as jnp
from jax import lax
from jax.experimental import pallas as pl
from jax.experimental.pallas import tpu as pltpu
from jax.sharding import PartitionSpec as P

HEAD_DIM = 64
PATTERNS = ((128, 1), (512, 4), (2048, 16))
REACH = 128
CLASSES = 16
LANES = 128
EPSILON = 1e-06
NEGATIVE = -1e30
GROUPS = 2


def attend_kernel(q_ref, k_ref, v_ref, o_ref, out_sc, top_sc, sum_sc, near_bias, mid_bias, far_bias):
    chunks, _, per_class, width = q_ref.shape
    heads = width // HEAD_DIM
    tile = 16
    near_rows = CLASSES * tile
    mid_rows = 4 * per_class
    span = REACH // per_class
    far_tiles = chunks // span

    def bias_of(diff, window, live):
        return jnp.where((diff >= 0) & (diff <= window) & live, 0.0, NEGATIVE).astype(jnp.float32)

    row = lax.broadcasted_iota(jnp.int32, near_bias.shape[1:], 0)
    col = lax.broadcasted_iota(jnp.int32, near_bias.shape[1:], 1)
    diff = (row % tile - col % tile) * 16 + row // tile - (col % near_rows) // tile
    diff = diff + jnp.where(col < near_rows, near_rows, 0)
    near_bias[0] = bias_of(diff, PATTERNS[0][0], col >= near_rows)
    near_bias[1] = bias_of(diff, PATTERNS[0][0], col >= 0)
    row = lax.broadcasted_iota(jnp.int32, mid_bias.shape[1:], 0)
    col = lax.broadcasted_iota(jnp.int32, mid_bias.shape[1:], 1)
    diff = (row % per_class - col % per_class) * 16
    diff = diff + 4 * (row // per_class - (col % mid_rows) // per_class)
    diff = diff + jnp.where(col < mid_rows, CLASSES * per_class, 0)
    mid_bias[0] = bias_of(diff, PATTERNS[1][0], col >= mid_rows)
    mid_bias[1] = bias_of(diff, PATTERNS[1][0], col >= 0)
    row = lax.broadcasted_iota(jnp.int32, far_bias.shape, 0)
    col = lax.broadcasted_iota(jnp.int32, far_bias.shape, 1)
    far_bias[...] = bias_of(row + REACH - col, REACH, col >= 0)

    lane = lax.broadcasted_iota(jnp.int32, (1, width), 1) // HEAD_DIM
    picks = [jnp.where(lane == h, HEAD_DIM ** -0.5, 0.0).astype(jnp.bfloat16) for h in range(heads)]

    def attend(queries, keys, values, bias):
        outs, tops, sums = [], [], []
        for h in range(heads):
            scores = lax.dot_general(
                queries * picks[h], keys, (((1,), (1,)), ((), ())), preferred_element_type=jnp.float32
            ) + bias
            top = jnp.max(scores, axis=1, keepdims=True)
            raised = jnp.exp(scores - top)
            total = jnp.sum(raised, axis=1, keepdims=True)
            outs.append(jnp.dot(raised.astype(jnp.bfloat16), values, preferred_element_type=jnp.float32))
            tops.append(jnp.broadcast_to(top, outs[-1].shape))
            sums.append(jnp.broadcast_to(total, outs[-1].shape))

        def join(parts):
            whole = parts[0]
            for h in range(1, heads):
                whole = jnp.where(lane == h, parts[h], whole)
            return whole

        return join(outs), join(tops), join(sums)

    def merge_rows(ref, *index):
        block = ref[index]
        return block.reshape(-1, width)

    @pl.loop(0, chunks)
    def near_and_mid(z):
        before = jnp.maximum(z - 1, 0)
        first = jnp.minimum(z, 1)
        for u in range(per_class // tile):
            rows = slice(u * tile, (u + 1) * tile)
            back, back_rows, kind = (before, slice(per_class - tile, per_class), first)
            if u > 0:
                back, back_rows, kind = (z, slice((u - 1) * tile, u * tile), 1)
            queries = q_ref[z, :, rows, :].reshape(near_rows, width)
            keys, values = (
                jnp.concatenate(
                    [
                        ref[back, :, back_rows, :].reshape(near_rows, width),
                        ref[z, :, rows, :].reshape(near_rows, width),
                    ],
                    axis=0,
                )
                for ref in (k_ref, v_ref)
            )
            for ref, part in zip((out_sc, top_sc, sum_sc), attend(queries, keys, values, near_bias[kind])):
                ref[0, z, :, rows, :] = part.reshape(CLASSES, tile, width)
        for r in range(4):
            classes = range(r, CLASSES, 4)
            queries = jnp.concatenate([q_ref[z, c] for c in classes], axis=0)
            keys, values = (
                jnp.concatenate([ref[y, c] for y in (before, z) for c in classes], axis=0)
                for ref in (k_ref, v_ref)
            )
            for ref, part in zip((out_sc, top_sc, sum_sc), attend(queries, keys, values, mid_bias[first])):
                for m, c in enumerate(classes):
                    ref[1, z, c] = part[m * per_class : (m + 1) * per_class]

    @pl.loop(0, CLASSES // 4)
    def far(quad):
        for inner in range(4):
            c = quad * 4 + inner
            for n in range(far_tiles):
                here = slice(n * span, (n + 1) * span)
                reach = slice(max(n - 1, 0) * span, (n + 1) * span)
                queries = q_ref[here, c].reshape(REACH, width)
                keys, values = (ref[reach, c].reshape(-1, width) for ref in (k_ref, v_ref))
                bias = far_bias[...] if n > 0 else far_bias[:, REACH:]
                for ref, part in zip((out_sc, top_sc, sum_sc), attend(queries, keys, values, bias)):
                    ref[2, here, c] = part.reshape(span, per_class, width)

    @pl.loop(0, chunks)
    def mix(z):
        tops = [top_sc[p, z] for p in range(3)]
        highest = jnp.maximum(jnp.maximum(tops[0], tops[1]), tops[2])
        lifts = [jnp.exp(top - highest) for top in tops]
        total = sum(lift * sum_sc[p, z] for p, lift in enumerate(lifts))
        result = sum(lift * out_sc[p, z] for p, lift in enumerate(lifts))
        o_ref[z] = (result / total).astype(o_ref.dtype)


def attend_all(moved, width):
    chunks, batches, _, per_class, triple = moved.shape
    channels = triple // 3
    pairs = channels // width
    if width % 128 == 0:
        operands = (moved, moved, moved)
        starts = (0, pairs, 2 * pairs)
    else:
        operands = tuple(moved[..., i * channels : (i + 1) * channels] for i in range(3))
        starts = (0, 0, 0)
    block = (chunks, None, CLASSES, per_class, width)
    tokens = chunks * CLASSES * per_class
    return pl.pallas_call(
        attend_kernel,
        grid=(batches, pairs),
        in_specs=[
            pl.BlockSpec(block, functools.partial(lambda s, b, i: (0, b, 0, 0, s + i), start)) for start in starts
        ],
        out_specs=pl.BlockSpec(block, lambda b, i: (0, b, 0, 0, i)),
        out_shape=jax.ShapeDtypeStruct((chunks, batches, CLASSES, per_class, channels), jnp.bfloat16),
        scratch_shapes=[pltpu.VMEM((3, chunks, CLASSES, per_class, width), jnp.float32) for _ in range(3)]
        + [
            pltpu.VMEM((2, 256, 512), jnp.float32),
            pltpu.VMEM((2, 4 * per_class, 8 * per_class), jnp.float32),
            pltpu.VMEM((REACH, 2 * REACH), jnp.float32),
        ],
        cost_estimate=pl.CostEstimate(
            flops=tokens * batches * channels * 4 * 900,
            bytes_accessed=tokens * batches * channels * 8,
            transcendentals=tokens * batches * channels // HEAD_DIM * 900,
        ),
    )(*operands)


def project_kernel(weight_count, places, tokens_ref, *refs):
    weight_refs, out_ref, product = refs[:weight_count], refs[weight_count], refs[-1]
    step = pl.program_id(0)
    positions, batch_size, features = tokens_ref.shape
    rows = positions * batch_size
    flat = tokens_ref[...].reshape(rows, features)
    at = pl.ds(pl.multiple_of(step * rows, rows), rows)
    for weight_ref, parts in zip(weight_refs, places):
        total = jnp.dot(flat, weight_ref[...], preferred_element_type=jnp.float32)
        for i, part in enumerate(parts):
            product[part, at, :] = total[:, i * LANES : (i + 1) * LANES]

    @pl.when(step == pl.num_programs(0) - 1)
    def leave():
        per_class = out_ref.shape[2]

        @pl.loop(0, CLASSES)
        def of_class(c):
            for part in range(product.shape[0]):
                for b in range(batch_size):
                    picked = pl.ds(c * batch_size + b, per_class, stride=CLASSES * batch_size)
                    out_ref[b, c, :, part * LANES : (part + 1) * LANES] = product[part, picked, :].astype(out_ref.dtype)


def project(tokens, weights, group, cut):
    seq_rows, batch_size, features = tokens.shape
    columns = cut * len(weights)
    per_class = seq_rows // CLASSES
    block = min(64, seq_rows)
    shape = (batch_size, CLASSES, per_class, columns)
    each = cut // LANES
    places = [range(w * each, (w + 1) * each) for w in range(len(weights))]
    return pl.pallas_call(
        functools.partial(project_kernel, len(weights), places),
        grid=(seq_rows // block,),
        in_specs=[pl.BlockSpec((block, batch_size, features), lambda i: (i, 0, 0))]
        + [pl.BlockSpec((features, cut), lambda i: (0, group))] * len(weights),
        out_specs=pl.BlockSpec(shape, lambda i: (0, 0, 0, 0)),
        out_shape=jax.ShapeDtypeStruct(shape, jnp.bfloat16),
        scratch_shapes=[pltpu.VMEM((columns // LANES, seq_rows * batch_size, LANES), jnp.float32)],
        compiler_params=pltpu.CompilerParams(dimension_semantics=("arbitrary",)),
        cost_estimate=pl.CostEstimate(
            flops=2 * seq_rows * batch_size * features * columns,
            bytes_accessed=2 * (tokens.size + features * columns + seq_rows * batch_size * columns),
            transcendentals=0,
        ),
    )(tokens, *weights)


STRIDE = PATTERNS[1][1]
MESH = pl.DeviceIdType.MESH


def layer_kernel(tokens_ref, *refs):
    in_weights, gain_ref, own_ref, out_ref = refs[:3], refs[3], refs[4], refs[5]
    (raw, kept, product, qkv_ref, in_sem, late_q, last_q, first_kv, back, back_norm, sent, sent_norm, held, held_norm, done, gathered, weights, gains, normed,
     mixed, diag_bias, class_bias, corner_bias, send_sem, recv_sem, part_send, part_recv, w_send, w_recv, out_sem) = refs[6:]
    place = lax.axis_index("sp")
    member = lax.axis_index("tp")
    blocks, depth, _, batch_size, features = tokens_ref.shape
    pieces = qkv_ref.shape[0]
    pairs = pieces // batch_size
    per = qkv_ref.shape[3]
    chunk = per * STRIDE
    tail = REACH // STRIDE
    members = gathered.shape[0]
    share = per // members
    half = LANES // 2

    def read_tokens(n, slot):
        return [
            pltpu.make_async_copy(tokens_ref.at[n, :, r], raw.at[slot, r], in_sem.at[slot, r]) for r in range(STRIDE)
        ]

    read_weights = [
        pltpu.make_async_copy(ref, kept.at[:, w * pairs * LANES : (w + 1) * pairs * LANES], in_sem.at[2, w])
        for w, ref in enumerate(in_weights)
    ]
    read_own = pltpu.make_async_copy(own_ref, weights.at[member], in_sem.at[2, 3])
    for c in read_tokens(0, 0) + read_weights + read_tokens(1, 1) + [read_own]:
        c.start()

    barrier = pltpu.get_barrier_semaphore()
    for other in range(1, 4):
        pl.semaphore_signal(barrier, inc=1, device_id={"sp": lax.rem(place + other, 4)}, device_id_type=MESH)
        pl.semaphore_signal(barrier, inc=1, device_id={"tp": member ^ other}, device_id_type=MESH)
    pl.semaphore_wait(barrier, 6)

    def to_place(kind, i, src, dst, target, axis="sp"):
        return pltpu.make_async_remote_copy(
            src_ref=src, dst_ref=dst, send_sem=send_sem.at[kind, i], recv_sem=recv_sem.at[kind, i],
            device_id={axis: target}, device_id_type=MESH,
        )

    def copy_kv(i, rows=slice(None)):
        return to_place(0, i, qkv_ref.at[i, pl.ds(1, 2), :, rows], first_kv.at[i, :, :, rows], 1)

    def copy_q2(i, rows=slice(None)):
        return to_place(1, i, qkv_ref.at[i, 0, :, rows], late_q.at[i, :, rows], 1)

    def copy_q3(i, target, rows=slice(None)):
        return to_place(1 + target, i, qkv_ref.at[i, 0, :, rows], last_q.at[i, :, rows], target)

    def copy_back(i, slot, source_slot, target):
        kind = 4 + target - 2 + 2 * slot
        return (
            to_place(kind, i, sent.at[source_slot, i], back.at[slot, i], target),
            to_place(kind + 4, i, sent_norm.at[source_slot, i], back_norm.at[slot, i], target),
        )

    def copy_part(i, x):
        rows = pl.ds(pl.multiple_of((member ^ x) * share, share), share)
        return pltpu.make_async_remote_copy(
            src_ref=done.at[i, :, rows], dst_ref=gathered.at[member, i],
            send_sem=part_send.at[x - 1, i], recv_sem=part_recv.at[x - 1, i],
            device_id={"tp": member ^ x}, device_id_type=MESH,
        )

    def copy_gain(x):
        return pltpu.make_async_remote_copy(
            src_ref=gain_ref, dst_ref=gains.at[member], send_sem=w_send.at[2 + x], recv_sem=w_recv.at[2 + x],
            device_id={"tp": member ^ x}, device_id_type=MESH,
        )

    def copy_weight(x, kind):
        src = own_ref if kind < 2 else weights.at[member ^ 2]
        dst = weights.at[member ^ 2 if kind == 2 else member]
        return pltpu.make_async_remote_copy(
            src_ref=src, dst_ref=dst, send_sem=w_send.at[kind], recv_sem=w_recv.at[kind],
            device_id={"tp": member ^ x}, device_id_type=MESH,
        )

    def send_early(i, rows=slice(None)):
        @pl.when(place == 0)
        def send_first():
            copy_kv(i, rows).start()

        @pl.when(place == 2)
        def send_late():
            copy_q2(i, rows).start()

        @pl.when(place == 3)
        def send_last():
            copy_q3(i, 1, rows).start()
            copy_q3(i, 2, rows).start()

    copy_weight(2, 0).start()
    copy_weight(1, 1).start()
    for x in range(1, members):
        copy_gain(x).start()

    def bias_of(diff, patterns):
        count = jnp.zeros(diff.shape, jnp.int32)
        for window, dilation in patterns:
            count += jnp.where((diff >= 0) & (diff <= window) & (diff % dilation == 0), 1, 0)
        logs = jnp.where(count == 2, 0.6931471805599453, jnp.where(count == 3, 1.0986122886681098, 0.0))
        return jnp.where(count == 0, NEGATIVE, logs).astype(jnp.float32)

    row = lax.broadcasted_iota(jnp.int32, (chunk, LANES), 0)
    col = lax.broadcasted_iota(jnp.int32, (chunk, LANES), 1)
    for r in range(STRIDE):
        diag_bias[r] = bias_of(STRIDE * (col - row % per) + r - row // per, PATTERNS)
        key = row[:REACH]
        back_by = STRIDE * (per - tail + key % tail) + key // tail
        corner_bias[r] = bias_of(chunk + STRIDE * col[:REACH] + r - back_by, PATTERNS[:1])
    for gap in range(2):
        class_bias[gap] = bias_of((gap + 1) * chunk + STRIDE * (col[:per] - row[:per]), PATTERNS[1:])

    early = min(2, pieces)
    for c in read_weights:
        c.wait()

    @pl.loop(0, blocks)
    def project(n):
        slot = lax.rem(n, 2)
        for c in read_tokens(n, slot):
            c.wait()
        flat = raw[slot].reshape(STRIDE * depth * batch_size, features)
        total = jnp.dot(flat, kept[...], preferred_element_type=jnp.float32)
        for part in range(3 * pairs):
            product[part] = total[:, part * LANES : (part + 1) * LANES]

        @pl.when(n + 2 < blocks)
        def read_ahead():
            for c in read_tokens(n + 2, slot):
                c.start()

        here = pl.ds(pl.multiple_of(n * depth, depth), depth)
        for b in range(batch_size):
            for which in range(3):
                for pair in range(pairs):
                    for r in range(STRIDE):
                        picked = pl.ds(r * depth * batch_size + b, depth, stride=batch_size)
                        qkv_ref[pair * batch_size + b, which, r, here] = product[
                            which * pairs + pair, picked
                        ].astype(jnp.bfloat16)
        for i in range(early):
            send_early(i, here)

    @pl.loop(early, pieces)
    def send_rest(i):
        send_early(i)

    read_own.wait()
    lane = lax.broadcasted_iota(jnp.int32, (1, LANES), 1) // HEAD_DIM
    picks = [jnp.where(lane == h, HEAD_DIM ** -0.5, 0.0).astype(jnp.bfloat16) for h in range(2)]
    eye = jnp.where(
        lax.broadcasted_iota(jnp.int32, (LANES, LANES), 0) == lax.broadcasted_iota(jnp.int32, (LANES, LANES), 1), 1.0, 0.0
    ).astype(jnp.bfloat16)

    def contract_last(a, b):
        return lax.dot_general(a, b, (((1,), (1,)), ((), ())), preferred_element_type=jnp.float32)

    def turn(a):
        return contract_last(eye, a).astype(jnp.bfloat16)

    def spread(two):
        return jnp.concatenate([jnp.broadcast_to(two[h : h + 1], (half, LANES)) for h in range(2)], axis=0)

    def attend(jobs):
        begun = []
        for queries, parts in jobs:
            both = jnp.concatenate([queries * picks[0], queries * picks[1]], axis=0)
            scores = []
            for keys, _, bias in parts:
                scores.append(contract_last(keys, both) + jnp.concatenate([bias, bias], axis=1))
            top = functools.reduce(jnp.maximum, [jnp.max(s, axis=0, keepdims=True) for s in scores])
            begun.append((scores, top, parts))
        mixed = []
        for scores, top, parts in begun:
            total, result = 0.0, 0.0
            for s, (_, turned, _) in zip(scores, parts):
                raised = jnp.exp(s - top)
                total += jnp.sum(raised, axis=0, keepdims=True)
                result += jnp.dot(turned, raised.astype(jnp.bfloat16), preferred_element_type=jnp.float32)
            mixed.append((result, top, total))
        answers = []
        for result, top, total in mixed:
            picked = jnp.concatenate([result[:half, :LANES], result[half:, LANES:]], axis=0)
            norm = top + jnp.log(total)
            inverse = 1.0 / total
            two = jnp.concatenate([inverse[:, :LANES], inverse[:, LANES:]], axis=0)
            answers.append((picked * spread(two), jnp.concatenate([norm[:, :LANES], norm[:, LANES:]], axis=0)))
        return answers

    def all_rows(block):
        return block.reshape(chunk, LANES)

    def cls(r):
        return slice(r * per, (r + 1) * per)

    def corner_of(rows):
        return jnp.concatenate([rows[r * per + per - tail : (r + 1) * per] for r in range(STRIDE)], axis=0)

    def finish(i, results):
        rows = [turn(result.astype(jnp.bfloat16)) for result in results]
        for r in range(STRIDE):
            done[i, r] = rows[r]

    def send_parts(i):
        mine = pl.ds(pl.multiple_of(member * share, share), share)
        gathered[member, i] = done[i, :, mine]
        for x in range(1, members):
            copy_part(i, x).start()

    def own_parts(i):
        return all_rows(qkv_ref[i, 1]), turn(all_rows(qkv_ref[i, 2]))

    def far_parts(keys, turned, r, gap):
        return keys[cls(r)], turned[:, cls(r)], class_bias[gap]

    def give_back(i, source_slot, answers):
        for r in range(STRIDE):
            sent[source_slot, i, :, cls(r)] = answers[r][0].astype(jnp.bfloat16)
            sent_norm[source_slot, i, :, cls(r)] = answers[r][1]

    def merge(i, sources):
        rows = []
        for r in range(STRIDE):
            norms = [held_norm[i, :, cls(r)]] + [back_norm[s, i, :, cls(r)] for s in sources]
            results = [held[i, :, cls(r)]] + [back[s, i, :, cls(r)].astype(jnp.float32) for s in sources]
            top = functools.reduce(jnp.maximum, norms)
            raised = [jnp.exp(n - top) for n in norms]
            inverse = 1.0 / sum(raised)
            rows.append(sum(spread(e * inverse) * o for e, o in zip(raised, results)))
        finish(i, rows)

    @pl.when(place >= 2)
    def later():
        @pl.loop(0, pieces)
        def one(i):
            keys, turned = own_parts(i)
            jobs = [(qkv_ref[i, 0, r], [(keys, turned, diag_bias[r])]) for r in range(STRIDE)]
            for r, (result, norm) in enumerate(attend(jobs)):
                held[i, :, cls(r)] = result
                held_norm[i, :, cls(r)] = norm

            @pl.when(place == 2)
            def help_last():
                near_keys = corner_of(all_rows(qkv_ref[i, 1]))
                near_turned = turn(corner_of(all_rows(qkv_ref[i, 2])))
                copy_q3(i, 2).wait_recv()
                jobs = []
                for r in range(STRIDE):
                    parts = [far_parts(keys, turned, r, 0), (near_keys, near_turned, corner_bias[r])]
                    jobs.append((last_q[i, r], parts))
                give_back(i, 0, attend(jobs))
                for c in copy_back(i, 1, 0, 3):
                    c.start()

    def first(i):
        keys, turned = own_parts(i)
        jobs = [(qkv_ref[i, 0, r], [(keys, turned, diag_bias[r])]) for r in range(STRIDE)]
        finish(i, [answer[0] for answer in attend(jobs)])

    def second(i):
        keys, turned = own_parts(i)
        near_keys = corner_of(keys)
        near_turned = turn(corner_of(all_rows(qkv_ref[i, 2])))
        copy_kv(i).wait_recv()
        old_keys, old_turned = all_rows(first_kv[i, 0]), turn(all_rows(first_kv[i, 1]))
        copy_q2(i).wait_recv()
        jobs = []
        for r in range(STRIDE):
            parts = [
                far_parts(keys, turned, r, 0),
                (near_keys, near_turned, corner_bias[r]),
                far_parts(old_keys, old_turned, r, 1),
            ]
            jobs.append((late_q[i, r], parts))
        give_back(i, 0, attend(jobs))
        for c in copy_back(i, 0, 0, 2):
            c.start()
        copy_q3(i, 1).wait_recv()
        jobs = []
        for r in range(STRIDE):
            parts = [far_parts(keys, turned, r, 1), far_parts(old_keys, old_turned, r, 1)]
            jobs.append((last_q[i, r], parts))
        give_back(i, 1, attend(jobs))
        for c in copy_back(i, 0, 1, 3):
            c.start()
        old_near_keys = corner_of(old_keys)
        old_near_turned = turn(corner_of(all_rows(first_kv[i, 1])))
        jobs = []
        for r in range(STRIDE):
            parts = [
                (keys, turned, diag_bias[r]),
                far_parts(old_keys, old_turned, r, 0),
                (old_near_keys, old_near_turned, corner_bias[r]),
            ]
            jobs.append((qkv_ref[i, 0, r], parts))
        finish(i, [answer[0] for answer in attend(jobs)])

    def third(i):
        for c in copy_back(i, 0, 0, 2):
            c.wait_recv()
        merge(i, (0,))

    def fourth(i):
        for c in copy_back(i, 0, 1, 3) + copy_back(i, 1, 0, 3):
            c.wait_recv()
        merge(i, (0, 1))

    rows = STRIDE * share
    width = pairs * LANES
    target = lax.broadcasted_iota(jnp.int32, (rows, rows), 0)
    source = lax.broadcasted_iota(jnp.int32, (rows, rows), 1)
    order = jnp.where(target == source % share * STRIDE + source // share, 1.0, 0.0).astype(jnp.bfloat16)

    def write_out(b):
        return pltpu.make_async_copy(mixed.at[b], out_ref.at[b], out_sem.at[b])

    def project_out(b):
        for pair in range(pairs):
            for x in range(1, members):
                copy_part(pair * batch_size + b, x).wait_recv()
        square = 0.0
        turned = []
        for t in range(members):
            for pair in range(pairs):
                block = gathered[t, pair * batch_size + b].reshape(rows, LANES)
                turned.append(jnp.dot(order, block, preferred_element_type=jnp.float32))
                square += turned[-1] * turned[-1]
        square = jnp.sum(square, axis=1, keepdims=True)
        scale = lax.rsqrt(square * (1.0 / (LANES * len(turned))) + EPSILON)
        for at, block in enumerate(turned):
            gain = gains[at // pairs, at % pairs : at % pairs + 1]
            normed[:, at * LANES : (at + 1) * LANES] = (block * scale * gain).astype(jnp.bfloat16)

        @pl.loop(0, mixed.shape[2] // (2 * LANES))
        def columns_of(n):
            columns = pl.ds(pl.multiple_of(n * 2 * LANES, 2 * LANES), 2 * LANES)
            total = 0.0
            for t in range(members):
                total += jnp.dot(
                    normed[:, t * width : (t + 1) * width], weights[t, :, columns], preferred_element_type=jnp.float32
                )
            mixed[b, :, columns] = total.astype(mixed.dtype)

        write_out(b).start()

    ready = (pairs - 1) * batch_size

    @pl.loop(0, pieces)
    def one(i):
        for role, complete in enumerate((first, second, third, fourth)):
            @pl.when(place == role)
            def run(complete=complete):
                complete(i)
        send_parts(i)

        @pl.when(i == pieces // 2 - 1)
        def forward():
            copy_weight(2, 0).wait_recv()
            copy_weight(1, 2).start()

        @pl.when(i == ready)
        def weights_here():
            copy_weight(1, 1).wait_recv()
            copy_weight(1, 2).wait_recv()
            for x in range(1, members):
                copy_gain(x).wait_recv()
            gains[member] = gain_ref[...]

        @pl.when(i > ready)
        def previous():
            project_out(i - ready - 1)

    project_out(batch_size - 1)

    @pl.when(place == 0)
    def first_sent():
        @pl.loop(0, pieces)
        def one(i):
            copy_kv(i).wait_send()

    @pl.when(place == 1)
    def second_sent():
        @pl.loop(0, pieces)
        def one(i):
            for c in copy_back(i, 0, 0, 2) + copy_back(i, 0, 1, 3):
                c.wait_send()

    @pl.when(place == 2)
    def third_sent():
        @pl.loop(0, pieces)
        def one(i):
            copy_q2(i).wait_send()
            for c in copy_back(i, 1, 0, 3):
                c.wait_send()

    @pl.when(place == 3)
    def fourth_sent():
        @pl.loop(0, pieces)
        def one(i):
            copy_q3(i, 1).wait_send()
            copy_q3(i, 2).wait_send()

    @pl.loop(0, pieces)
    def parts_sent(i):
        for x in range(1, members):
            copy_part(i, x).wait_send()

    for x, kind in ((2, 0), (1, 1), (1, 2)):
        copy_weight(x, kind).wait_send()
    for x in range(1, members):
        copy_gain(x).wait_send()
    for b in range(batch_size):
        write_out(b).wait()


def four_chunks(tokens, query_weight, key_weight, value_weight, mix_gain, out_weight):
    chunk, batch_size, features = tokens.shape
    width, columns = out_weight.shape
    members = lax.axis_size("tp")
    pairs = width // LANES
    pieces = pairs * batch_size
    per = chunk // STRIDE
    depth = 16
    rows = chunk // members
    bf16, f32 = jnp.bfloat16, jnp.float32
    sems = pltpu.SemaphoreType.DMA
    scratch = [
        pltpu.VMEM((2, STRIDE, depth, batch_size, features), bf16),
        pltpu.VMEM((features, 3 * width), bf16),
        pltpu.VMEM((3 * pairs, STRIDE * depth * batch_size, LANES), f32),
        pltpu.VMEM((pieces, 3, STRIDE, per, LANES), bf16),
        sems((3, STRIDE)),
        pltpu.VMEM((pieces, STRIDE, per, LANES), bf16),
        pltpu.VMEM((pieces, STRIDE, per, LANES), bf16),
        pltpu.VMEM((pieces, 2, STRIDE, per, LANES), bf16),
        pltpu.VMEM((2, pieces, LANES, chunk), bf16),
        pltpu.VMEM((2, pieces, 2, chunk), f32),
        pltpu.VMEM((2, pieces, LANES, chunk), bf16),
        pltpu.VMEM((2, pieces, 2, chunk), f32),
        pltpu.VMEM((pieces, LANES, chunk), f32),
        pltpu.VMEM((pieces, 2, chunk), f32),
        pltpu.VMEM((pieces, STRIDE, per, LANES), bf16),
        pltpu.VMEM((members, pieces, STRIDE, per // members, LANES), bf16),
        pltpu.VMEM((members, width, columns), bf16),
        pltpu.VMEM((members, pairs, LANES), f32),
        pltpu.VMEM((rows, width * members), bf16),
        pltpu.VMEM((batch_size, rows, columns), bf16),
        pltpu.VMEM((STRIDE, chunk, LANES), f32),
        pltpu.VMEM((2, per, LANES), f32),
        pltpu.VMEM((STRIDE, REACH, LANES), f32),
        sems((12, pieces)),
        sems((12, pieces)),
        sems((members - 1, pieces)),
        sems((members - 1, pieces)),
        sems((2 + members,)),
        sems((2 + members,)),
        sems((batch_size,)),
    ]
    mixed = pl.pallas_call(
        layer_kernel,
        in_specs=[pl.BlockSpec(memory_space=pl.ANY)] * 4
        + [pl.BlockSpec(memory_space=pltpu.VMEM), pl.BlockSpec(memory_space=pl.ANY)],
        out_specs=pl.BlockSpec(memory_space=pl.ANY),
        out_shape=jax.ShapeDtypeStruct((batch_size, rows, columns), bf16),
        scratch_shapes=scratch,
        compiler_params=pltpu.CompilerParams(collective_id=0, has_side_effects=True),
        cost_estimate=pl.CostEstimate(
            flops=6 * tokens.size * width, bytes_accessed=4 * tokens.size, transcendentals=tokens.size * 100
        ),
    )(
        tokens.reshape(per // depth, depth, STRIDE, batch_size, features),
        query_weight,
        key_weight,
        value_weight,
        mix_gain.reshape(pairs, LANES),
        out_weight,
    )
    return mixed.transpose(1, 0, 2)


def fits_four_chunks(tokens, query_weight):
    return (
        lax.axis_size("sp") == 4
        and lax.axis_size("tp") == 4
        and tokens.shape[0] == STRIDE * LANES
        and tokens.shape[0] == PATTERNS[1][0]
        and 4 * tokens.shape[0] <= PATTERNS[2][0]
        and query_weight.shape[1] % LANES == 0
    )


def body(tokens, query_weight, key_weight, value_weight, mix_gain, out_weight):
    if fits_four_chunks(tokens, query_weight):
        return four_chunks(tokens, query_weight, key_weight, value_weight, mix_gain, out_weight)
    seq_rows, batch_size, features = tokens.shape
    channels = query_weight.shape[1]
    sp_count = lax.axis_size("sp")
    tp_count = lax.axis_size("tp")
    tp_place = lax.axis_index("tp")
    per_class = seq_rows // CLASSES
    head_split = min(max(1, sp_count // batch_size), channels // HEAD_DIM)
    copies = max(1, sp_count // (batch_size * head_split))
    batches = max(1, batch_size // sp_count)
    groups = GROUPS if head_split == 1 else 1

    own = (out_weight.astype(jnp.float32) * mix_gain[:, None]).astype(jnp.bfloat16)
    gathered, sources, step = own, [0], tp_count // 2
    while step:
        route = [(i, i ^ step) for i in range(tp_count)]
        gathered = jnp.concatenate([gathered, lax.ppermute(gathered, "tp", route)], axis=0)
        sources += [s ^ step for s in sources]
        step //= 2

    cut = channels // groups // head_split
    width = min(cut, 2 * HEAD_DIM)
    weights = (query_weight, key_weight, value_weight)
    results = []
    for g in range(groups):
        if cut % LANES == 0 and head_split == 1:
            product = project(tokens, weights, g, cut)
        else:
            spans = [slice(i * cut, (i + 1) * cut) for i in range(g * head_split, (g + 1) * head_split)]
            whole = jnp.concatenate([w[:, span] for span in spans for w in weights], axis=1)
            product = project(tokens, (whole,), 0, whole.shape[1])
        if head_split > 1:
            product = product.reshape(batch_size, seq_rows, head_split, 3 * cut).transpose(0, 2, 1, 3)
        product = product.reshape(sp_count // copies, batches * seq_rows, 3 * cut)
        if copies > 1:
            product = jnp.repeat(product, copies, axis=0)
        moved = lax.all_to_all(product, "sp", split_axis=0, concat_axis=0, tiled=True)
        if g == 0:
            moved, gathered = lax.optimization_barrier((moved, gathered))
        moved = moved.reshape(sp_count, batches, CLASSES, per_class, 3 * cut)
        results.append(attend_all(moved, width))

    part = per_class // tp_count
    backs = []
    for result in results:
        back = result.reshape(sp_count, batches, CLASSES, tp_count, part, cut).transpose(0, 3, 1, 2, 4, 5)
        back = back.reshape(sp_count * tp_count, batches * CLASSES * part, cut)
        back = lax.all_to_all(back, ("sp", "tp"), split_axis=0, concat_axis=0, tiled=True)
        back = back.reshape(batch_size // batches, head_split, copies, tp_count, batches, CLASSES, part, cut)[:, :, 0]
        backs.append(back)
    combined = jnp.stack(backs, axis=0).transpose(3, 6, 5, 1, 4, 0, 2, 7)
    rows = part * CLASSES * batch_size
    combined = combined.reshape(tp_count, rows, channels)
    turned = jnp.concatenate(
        [lax.dynamic_index_in_dim(combined, tp_place ^ s, axis=0, keepdims=False) for s in sources], axis=1
    )
    wide = turned.astype(jnp.float32)
    row_scale = lax.rsqrt(jnp.mean(wide * wide, axis=-1, keepdims=True) + EPSILON)
    mixed = jnp.dot(turned, gathered, preferred_element_type=jnp.float32) * row_scale
    return mixed.astype(jnp.bfloat16).reshape(part * CLASSES, batch_size, out_weight.shape[1])


def solution(mesh):
    in_specs = (
        P("sp", "grp", None),
        P(None, "tp"),
        P(None, "tp"),
        P(None, "tp"),
        P("tp"),
        P("tp", None),
    )
    out_specs = P(("sp", "tp"), "grp", None)
    return jax.shard_map(body, mesh=mesh, in_specs=in_specs, out_specs=out_specs, check_vma=False)
```
